32 devices in a mesh: ep: 8 (over z, x), tp: 4 (over y, core).
Axes of the slice: x: 2, y: 2, z: 4, core: 2. Of those that a mesh axis runs over, the one named last changes fastest.
Arguments:
- queries: bfloat16 [1024, 4096], P('ep', 'tp'), may hold values from -6 to 6
- key_rows: bfloat16 [1024, 4096], P('ep', 'tp'), may hold values from -6 to 6
- value_rows: bfloat16 [1024, 4096], P('ep', 'tp'), may hold values from -6 to 6
- key_shift: bfloat16 [1024, 64], P('ep', 'tp'), may hold values from -20 to 1
- out_weight: bfloat16 [4096, 4096], P('tp'), may hold values from -0.09375 to 0.09375
- routed_rows: bfloat16 [1024, 4096], P('ep'), may hold values from -6 to 6
- expert_ids: int32 [1024, 2], P('ep'), may hold values from 0 to 7, as said below
- route_weights: float32 [1024, 2], P(('ep', 'tp')), may hold values from 0.2 to 1
- gate_weight: bfloat16 [8, 4096, 1024], P('ep', None, 'tp'), may hold values from -0.09375 to 0.09375
- up_weight: bfloat16 [8, 4096, 1024], P('ep', None, 'tp'), may hold values from -0.09375 to 0.09375
- down_weight: bfloat16 [8, 1024, 4096], P('ep', 'tp'), may hold values from -0.1875 to 0.1875
Outputs:
- mixed_rows: bfloat16 [1024, 4096], P(('ep', 'tp'))
- routed_out: bfloat16 [1024, 4096], P(('ep', 'tp'))
The draws below stay inside these ranges and needn't reach their ends.
Inputs may be any that keep to these rules, and one draw needn't show every extreme that they name: `expert_ids`: the two ids of a token differ and lie in one group of 2 consecutive experts. Within each aligned block of 32 tokens no expert is named more than 16 times.
All inputs are finite; a program needn't handle non-finite values.
Results may differ from the reference program's by a relative error of at most 0.015.
Values may be sent and summed in bfloat16 or wider, within the bound.
A program may use at most 128 MiB of HBM per device.

```python
import math
import jax
import jax.numpy as jnp
from jax import lax

D = 4096
HEAD_TOTAL = 64
HEAD = 64
FF = 1024
GROUPS = 4
KEY_BLOCK = 512
TOK_EP = 128
SEQUENCE_LENGTH = 1024
EXPERTS = 8
GROUP_SIZE = 2
SUB = 32
CAP = 16
N_TP = 4


def draw_key_shift(key, part):
    quick_key, offset_key, jitter_key, spike_key, level_key = jax.random.split(key, 5)
    fast_share = 0.5
    spike_rate = 2.0 / SEQUENCE_LENGTH
    quick_heads = jax.random.bernoulli(quick_key, fast_share, (HEAD_TOTAL,))
    baseline_level = jnp.where(quick_heads, -6.0, -math.log(SEQUENCE_LENGTH) - 0.5)
    block_start_offset = jnp.repeat(jax.random.uniform(offset_key, (SEQUENCE_LENGTH // TOK_EP, HEAD_TOTAL), jnp.float32, -0.7, 0.7), TOK_EP, axis=0)
    jitter_amount = jax.random.uniform(jitter_key, (SEQUENCE_LENGTH, HEAD_TOTAL), jnp.float32, -0.5, 0.5)
    spike_values = jax.random.bernoulli(spike_key, spike_rate, (SEQUENCE_LENGTH, HEAD_TOTAL)) & jnp.logical_not(quick_heads)[None, :]
    spike_level = jax.random.uniform(level_key, (SEQUENCE_LENGTH, HEAD_TOTAL), jnp.float32, -1.6, -0.7)
    shifted_values = jnp.where(spike_values, spike_level, baseline_level[None, :] + block_start_offset + jitter_amount)
    return shifted_values.astype(jnp.bfloat16)


def draw_expert_ids(key, part):
    full_group = jax.random.randint(jax.random.fold_in(key, 1), (), 0, GROUPS)
    table = jnp.array([[4, 2, 2], [3, 3, 2], [8, 0, 0], [6, 2, 0], [5, 3, 0]], jnp.int32)
    rest = SUB // 2

    def one_block(block_key):
        key_pattern, key_rank, key_order, key_cycle = jax.random.split(block_key, 4)
        pattern = table[jax.random.randint(key_pattern, (), 0, 5)] * (rest // 8)
        ranking = jax.random.permutation(key_rank, GROUPS)
        ranking = jnp.where(jnp.arange(GROUPS, dtype=jnp.int32) == full_group, GROUPS, ranking)
        ordering = jnp.argsort(ranking, stable=True)
        counts = jnp.zeros((GROUPS,), jnp.int32).at[ordering[:GROUPS - 1]].set(pattern)
        counts = counts.at[full_group].set(SUB // 2)
        bounds = jnp.cumsum(counts)
        places = jnp.arange(SUB, dtype=jnp.int32)
        labels = jnp.sum((places[:, None] >= bounds[None, :]).astype(jnp.int32), axis=1)
        within = places - (bounds - counts)[labels]
        shuffle = jax.random.permutation(key_order, SUB)
        labels = labels[shuffle]
        within = within[shuffle]
        cycle_keys = jax.random.split(key_cycle, GROUPS * CAP)
        cycles = jax.vmap(lambda cycle_key: jax.random.permutation(cycle_key, GROUP_SIZE))(cycle_keys)
        cycles = cycles.reshape(GROUPS, CAP, GROUP_SIZE)
        cycle_index = 2 * within // GROUP_SIZE
        place_index = 2 * within % GROUP_SIZE
        first_pick = cycles[labels, cycle_index, place_index]
        second_pick = cycles[labels, cycle_index, place_index + 1]
        return jnp.stack([labels * GROUP_SIZE + first_pick, labels * GROUP_SIZE + second_pick], axis=1).astype(jnp.int32)
    block_keys = jax.random.split(jax.random.fold_in(key, 2), SEQUENCE_LENGTH // SUB)
    return jax.vmap(one_block)(block_keys).reshape(SEQUENCE_LENGTH, 2)


def block_scale(rng, extent, shards, low, largest):
    def one(axis_at, blocks):
        draws = jax.random.uniform(jax.random.fold_in(jax.random.fold_in(rng, 6), axis_at), (blocks,), jnp.float32, low / len(shards), largest / len(shards))
        return jnp.repeat(jnp.exp(draws), extent[axis_at] // blocks).reshape((-1,) + (1,) * (len(extent) - axis_at - 1))

    gain = one(*shards[0])
    for cut in shards[1:]:
        gain = gain * one(*cut)
    return gain


def centred(key, dims, scale, reach, cuts=(), held_as=jnp.bfloat16):
    values = scale * jax.random.normal(key, dims, jnp.float32)
    if cuts:
        values = values * block_scale(key, dims, cuts, -0.22, 0.18)
    return jnp.clip(values, -reach, reach).astype(held_as)


def setup_inputs(seed: int = 0) -> dict:
    keys = jax.random.split(jax.random.key(seed), 12)
    return {
        "queries": centred(keys[0], (SEQUENCE_LENGTH, HEAD_TOTAL * HEAD), 1.0, 6.0, ((0, 8), (1, 4))),
        "key_rows": centred(keys[1], (SEQUENCE_LENGTH, HEAD_TOTAL * HEAD), 1.0, 6.0, ((0, 8), (1, 4))),
        "value_rows": centred(keys[2], (SEQUENCE_LENGTH, HEAD_TOTAL * HEAD), 1.0, 6.0, ((0, 8), (1, 4))),
        "key_shift": draw_key_shift(jax.random.fold_in(keys[11], 71), 0),
        "out_weight": centred(keys[4], (HEAD_TOTAL * HEAD, D), (HEAD_TOTAL * HEAD) ** -0.5, 0.09375, ((0, 4),)),
        "routed_rows": centred(keys[5], (SEQUENCE_LENGTH, D), 1.0, 6.0, ((0, 8),)),
        "expert_ids": draw_expert_ids(jax.random.fold_in(keys[11], 71), 0),
        "route_weights": jnp.clip(0.2 + 0.8 * jax.random.uniform(keys[7], (SEQUENCE_LENGTH, 2), jnp.float32) ** block_scale(keys[7], (SEQUENCE_LENGTH, 2), ((0, 32),), -0.2, 0.2), 0.2, 1.0),
        "gate_weight": centred(keys[8], (EXPERTS, D, FF), D ** -0.5, 0.09375, ((0, 8), (2, 4))),
        "up_weight": centred(keys[9], (EXPERTS, D, FF), D ** -0.5, 0.09375, ((0, 8), (2, 4))),
        "down_weight": centred(keys[10], (EXPERTS, FF, D), FF ** -0.5, 0.1875, ((0, 8), (1, 4))),
    }


def stick_attend(query_rows, key_all, value_all, shift_all, first_pos):
    row_count = query_rows.shape[0]
    head_count = query_rows.shape[1]
    head_depth = query_rows.shape[2]
    query_pos = first_pos + jnp.arange(row_count, dtype=jnp.int32)
    last_block = (first_pos + row_count - 1) // KEY_BLOCK
    score_scale = head_depth ** -0.5
    query_float = query_rows.astype(jnp.float32)

    def sweep_block(step_index, state_pair):
        running, logsum = state_pair
        row_start = ((last_block - step_index) * KEY_BLOCK).astype(jnp.int32)
        key_tile_block = lax.dynamic_slice_in_dim(key_all, row_start, KEY_BLOCK, 0).astype(jnp.float32)
        value_block = lax.dynamic_slice_in_dim(value_all, row_start, KEY_BLOCK, 0).astype(jnp.float32)
        shift_block = lax.dynamic_slice_in_dim(shift_all, row_start, KEY_BLOCK, 0).astype(jnp.float32)
        scores = jnp.einsum("thd,shd->hts", query_float, key_tile_block) * score_scale + shift_block.T[:, None, :]
        key_pos = row_start + jnp.arange(KEY_BLOCK, dtype=jnp.int32)
        strict = (key_pos[None, :] < query_pos[:, None])[None]
        log_keep = jnp.where(strict, jax.nn.log_sigmoid(-scores), 0.0)
        suffix = lax.cumsum(log_keep, axis=2, reverse=True) - log_keep + logsum[:, :, None]
        weight = jnp.where(strict, jnp.exp(jax.nn.log_sigmoid(scores) + suffix), 0.0).astype(jnp.bfloat16)
        running = running + jnp.einsum("hts,shd->htd", weight.astype(jnp.float32), value_block)
        return running, logsum + jnp.sum(log_keep, axis=2)

    initial = (jnp.zeros((head_count, row_count, head_depth), jnp.float32),
               jnp.zeros((head_count, row_count), jnp.float32))
    running, logsum = lax.fori_loop(0, last_block + 1, sweep_block, initial)
    return jnp.transpose(running, (1, 0, 2)).reshape(row_count, head_count * head_depth).astype(jnp.bfloat16)


def slot_numbers(pair_ids, expert_count):
    one_hot = (pair_ids[..., None] == jnp.arange(expert_count, dtype=jnp.int32)).astype(jnp.int32)
    earlier = jnp.cumsum(one_hot, axis=1) - one_hot
    return jnp.sum(one_hot * earlier, axis=2)


def reference(queries, key_rows, value_rows, key_shift, out_weight, routed_rows, expert_ids,
              route_weights, gate_weight, up_weight, down_weight):
    query_heads = queries.reshape(SEQUENCE_LENGTH, HEAD_TOTAL, HEAD)
    key_heads = key_rows.reshape(SEQUENCE_LENGTH, HEAD_TOTAL, HEAD)
    value_heads = value_rows.reshape(SEQUENCE_LENGTH, HEAD_TOTAL, HEAD)
    block_count = SEQUENCE_LENGTH // KEY_BLOCK

    def one_block(pair):
        query_block, block_index = pair
        return stick_attend(query_block, key_heads, value_heads, key_shift, block_index * KEY_BLOCK)

    attended = lax.map(one_block, (query_heads.reshape(block_count, KEY_BLOCK, HEAD_TOTAL, HEAD),
                                   jnp.arange(block_count, dtype=jnp.int32)))
    attended = attended.reshape(SEQUENCE_LENGTH, HEAD_TOTAL * HEAD)
    group_cols = HEAD_TOTAL * HEAD // N_TP
    mixed_sum = jnp.zeros((SEQUENCE_LENGTH, D), jnp.float32)
    for group in range(N_TP):
        partial_value = jnp.dot(attended[:, group * group_cols:(group + 1) * group_cols],
                          out_weight[group * group_cols:(group + 1) * group_cols],
                          preferred_element_type=jnp.float32).astype(jnp.bfloat16)
        partial_value = lax.optimization_barrier(partial_value)
        mixed_sum = mixed_sum + partial_value.astype(jnp.float32)
    mixed_rows = mixed_sum.astype(jnp.bfloat16)

    sub_count = SEQUENCE_LENGTH // SUB
    pair_ids = expert_ids.reshape(sub_count, SUB * 2)
    slots = slot_numbers(pair_ids, EXPERTS)
    block_ids = jnp.arange(sub_count, dtype=jnp.int32)[:, None]
    position = (block_ids * CAP + slots).reshape(-1)
    flat_ids = pair_ids.reshape(-1)
    token_index = jnp.arange(SEQUENCE_LENGTH * 2, dtype=jnp.int32) // 2
    dispatched = jnp.zeros((EXPERTS, sub_count * CAP, D), jnp.bfloat16)
    dispatched = dispatched.at[flat_ids, position].set(routed_rows[token_index])
    unit_group = FF // N_TP

    def one_expert(operands):
        expert_rows, gate_part, up_part, down_part = operands
        gate_proj = jnp.dot(expert_rows, gate_part, preferred_element_type=jnp.float32)
        up_proj = jnp.dot(expert_rows, up_part, preferred_element_type=jnp.float32)
        hidden = (jax.nn.silu(gate_proj) * up_proj).astype(jnp.bfloat16)
        summed = jnp.zeros((expert_rows.shape[0], D), jnp.float32)
        for group in range(N_TP):
            partial_value = jnp.dot(hidden[:, group * unit_group:(group + 1) * unit_group],
                              down_part[group * unit_group:(group + 1) * unit_group],
                              preferred_element_type=jnp.float32).astype(jnp.bfloat16)
            partial_value = lax.optimization_barrier(partial_value)
            summed = summed + partial_value.astype(jnp.float32)
        return summed.astype(jnp.bfloat16)

    expert_out = lax.map(one_expert, (dispatched, gate_weight, up_weight, down_weight))
    picked = expert_out[flat_ids, position].reshape(SEQUENCE_LENGTH, 2, D).astype(jnp.float32)
    routed_out = (picked[:, 0] * route_weights[:, 0:1] + picked[:, 1] * route_weights[:, 1:2]).astype(jnp.bfloat16)
    return mixed_rows, routed_out
```

```python
import jax
import jax.numpy as jnp
from jax import lax
from jax.experimental import pallas as pl
from jax.experimental.pallas import tpu as pltpu
from jax.sharding import PartitionSpec as P

HEAD = 64
KEY_BLOCK = 512
GROUPS = 4
TILE = 256
MESH = pl.DeviceIdType.MESH


def stick_attend(query_rows, key_all, value_all, shift_all, first_pos):
    row_count = query_rows.shape[0]
    head_count = query_rows.shape[1]
    head_depth = query_rows.shape[2]
    query_pos = first_pos + jnp.arange(row_count, dtype=jnp.int32)
    last_block = (first_pos + row_count - 1) // KEY_BLOCK
    score_scale = head_depth ** (-0.5)

    def sweep_block(step_index, state_pair):
        running, logsum = state_pair
        row_start = (last_block - step_index) * KEY_BLOCK
        key_tile_block = lax.dynamic_slice_in_dim(key_all, row_start, KEY_BLOCK, 0).reshape(
            KEY_BLOCK, head_count, head_depth
        )
        value_block = lax.dynamic_slice_in_dim(value_all, row_start, KEY_BLOCK, 0).reshape(
            KEY_BLOCK, head_count, head_depth
        )
        shift_block = lax.dynamic_slice_in_dim(shift_all, row_start, KEY_BLOCK, 0).astype(
            jnp.float32
        )
        scores = (
            jnp.einsum(
                "thd,shd->hts", query_rows, key_tile_block, preferred_element_type=jnp.float32
            )
            * score_scale
        )
        scores = scores + shift_block.T[:, None, :]
        key_pos = row_start + jnp.arange(KEY_BLOCK, dtype=jnp.int32)
        strict = (key_pos[None, :] < query_pos[:, None])[None]
        log_keep = jnp.where(strict, jax.nn.log_sigmoid(-scores), 0.0)
        suffix = lax.cumsum(log_keep, axis=2, reverse=True) - log_keep + logsum[:, :, None]
        weight = jnp.where(strict, jnp.exp(jax.nn.log_sigmoid(scores) + suffix), 0.0).astype(
            jnp.bfloat16
        )
        running = running + jnp.einsum(
            "hts,shd->htd", weight, value_block, preferred_element_type=jnp.float32
        )
        return (running, logsum + jnp.sum(log_keep, axis=2))

    initial = (
        jnp.zeros((head_count, row_count, head_depth), jnp.float32),
        jnp.zeros((head_count, row_count), jnp.float32),
    )
    running, logsum = lax.fori_loop(0, last_block + 1, sweep_block, initial)
    return (
        jnp.transpose(running, (1, 0, 2))
        .reshape(row_count, head_count * head_depth)
        .astype(jnp.bfloat16)
    )


def slot_numbers(pair_ids, expert_count):
    one_hot = (pair_ids[..., None] == jnp.arange(expert_count, dtype=jnp.int32)).astype(jnp.int32)
    earlier = jnp.cumsum(one_hot, axis=1) - one_hot
    return jnp.sum(one_hot * earlier, axis=2)


def pack_rows(source_rows, destination, slot_count):
    pair_count = destination.shape[0]
    matches = destination[None, :] == jnp.arange(slot_count, dtype=jnp.int32)[:, None]
    source_index = jnp.sum(
        jnp.where(matches, jnp.arange(pair_count, dtype=jnp.int32)[None, :] // 2, 0), axis=1
    )
    filled = jnp.any(matches, axis=1)
    picked = jnp.take(source_rows, source_index, axis=0)
    return jnp.where(filled[:, None], picked, jnp.zeros_like(picked))


def expand(expert_rows, gate_part, up_part):
    gate_proj = jnp.einsum(
        "rcd,df->rcf", expert_rows, gate_part, preferred_element_type=jnp.float32
    )
    up_proj = jnp.einsum("rcd,df->rcf", expert_rows, up_part, preferred_element_type=jnp.float32)
    return (jax.nn.silu(gate_proj) * up_proj).astype(jnp.bfloat16)


def meet(devices):
    barrier = pltpu.get_barrier_semaphore()
    for ep_to, tp_to in devices:
        pl.semaphore_signal(
            barrier, inc=1, device_id={"ep": ep_to, "tp": tp_to}, device_id_type=MESH
        )
    pl.semaphore_wait(barrier, len(devices))


def push(src, dst, send, recv, ep_to, tp_to):
    copy = pltpu.make_async_remote_copy(
        src_ref=src,
        dst_ref=dst,
        send_sem=send,
        recv_sem=recv,
        device_id={"ep": ep_to, "tp": tp_to},
        device_id_type=MESH,
    )
    copy.start()
    return copy


def spread_kernel(
    ep_count, q_ref, k_ref, v_ref, s_ref, rows_ref, qkv_ref, shift_ref, gath_ref,
    send_a, recv_a, send_b, recv_b, own_sem, block_sem,
):
    e = lax.axis_index("ep")
    t = lax.axis_index("tp")
    g = e // 2
    x = e % 2
    e_x = g * 2 + (1 - x)
    t_y = (t + 2) % 4
    t_c = t + 1 - 2 * (t % 2)
    t_yc = (t_c + 2) % 4
    block = q_ref.shape[0]
    width = q_ref.shape[1] // ep_count
    peers = [((e + d) % ep_count, t) for d in range(1, ep_count)]
    meet(peers + [(e, t_y), (e, t_c)])

    sends = []

    def forward(z, xi, ti, ep_to, tp_to):
        place = gath_ref.at[z, xi, ti]
        sends.append(
            push(place, place, send_b.at[len(sends)], recv_b.at[z, xi, ti], ep_to, tp_to)
        )

    def arrived(z, xi, ti):
        place = gath_ref.at[z, xi, ti]
        pltpu.make_async_copy(place, place, recv_b.at[z, xi, ti]).wait()

    for dz in (3, 2, 1):
        to = (g + dz) % GROUPS
        sends.append(
            push(
                rows_ref.at[to],
                gath_ref.at[g, x, t],
                send_b.at[len(sends)],
                recv_b.at[g, x, t],
                to * 2 + x,
                t,
            )
        )
    for ep_to, tp_to in ((e_x, t), (e, t_y), (e, t_c)):
        sends.append(
            push(
                rows_ref.at[g],
                gath_ref.at[g, x, t],
                send_b.at[len(sends)],
                recv_b.at[g, x, t],
                ep_to,
                tp_to,
            )
        )
    keep = pltpu.make_async_copy(rows_ref.at[g], gath_ref.at[g, x, t], block_sem)
    keep.start()
    exchange = []
    owns = []
    mine = pl.ds(pl.multiple_of(e * width, width), width)
    here = pl.ds(pl.multiple_of(e * block, block), block)
    for i, ref in enumerate((q_ref, k_ref, v_ref)):
        own = pltpu.make_async_copy(ref.at[:, mine], qkv_ref.at[i, here], own_sem.at[i])
        own.start()
        owns.append(own)
    own = pltpu.make_async_copy(s_ref.at[e], shift_ref.at[e], own_sem.at[3])
    own.start()
    owns.append(own)
    for d in range(1, ep_count):
        to = (e + d) % ep_count
        cols = pl.ds(pl.multiple_of(to * width, width), width)
        for i, ref in enumerate((q_ref, k_ref, v_ref)):
            exchange.append(
                push(
                    ref.at[:, cols],
                    qkv_ref.at[i, here],
                    send_a.at[i, d - 1],
                    recv_a.at[i, d - 1],
                    to,
                    t,
                )
            )
        exchange.append(
            push(
                s_ref.at[to], shift_ref.at[e], send_a.at[3, d - 1], recv_a.at[3, d - 1], to, t
            )
        )
    order = (0, 3, 1, 2)
    for dz in order[1:]:
        z = (g + dz) % GROUPS
        arrived(z, x, t)
        forward(z, x, t, e_x, t)
        forward(z, x, t, e, t_y)
        forward(z, x, t, e, t_c)
    for dz in order:
        z = (g + dz) % GROUPS
        arrived(z, 1 - x, t)
        if dz in (0, 3):
            forward(z, 1 - x, t, e, t_y)
        forward(z, 1 - x, t, e, t_c)
        arrived(z, x, t_y)
        if dz not in (0, 3):
            forward(z, x, t_y, e_x, t)
        forward(z, x, t_y, e, t_c)
    for dz in order:
        z = (g + dz) % GROUPS
        arrived(z, 1 - x, t_y)
        forward(z, 1 - x, t_y, e, t_c)
    for dz in order:
        z = (g + dz) % GROUPS
        for xi in (x, 1 - x):
            arrived(z, xi, t_c)
            arrived(z, xi, t_yc)
    for copy in exchange:
        copy.wait()
    for copy in sends:
        copy.wait_send()
    keep.wait()
    for copy in owns:
        copy.wait()


def spread(q, k, v, shift_rows, rows, ep_count, tp_count):
    block = q.shape[0]
    width = q.shape[1] // ep_count
    slots, row_width = rows.shape[1:]
    any_spec = pl.BlockSpec(memory_space=pl.ANY)
    vmem_spec = pl.BlockSpec(memory_space=pltpu.VMEM)

    def kernel(*refs):
        spread_kernel(ep_count, *refs)

    return pl.pallas_call(
        kernel,
        out_shape=(
            jax.ShapeDtypeStruct((3, block * ep_count, width), jnp.bfloat16),
            jax.ShapeDtypeStruct(shift_rows.shape, jnp.float32),
            jax.ShapeDtypeStruct((GROUPS, 2, tp_count, slots, row_width), jnp.bfloat16),
        ),
        in_specs=[vmem_spec] * 5,
        out_specs=(any_spec,) * 3,
        scratch_shapes=[
            pltpu.SemaphoreType.DMA((4, ep_count - 1)),
            pltpu.SemaphoreType.DMA((4, ep_count - 1)),
            pltpu.SemaphoreType.DMA((31,)),
            pltpu.SemaphoreType.DMA((GROUPS, 2, tp_count)),
            pltpu.SemaphoreType.DMA((4,)),
            pltpu.SemaphoreType.DMA,
        ],
        compiler_params=pltpu.CompilerParams(collective_id=0, has_side_effects=True),
    )(q, k, v, shift_rows, rows)


def stick_kernel(qkv_ref, shift_ref, tri_ref, out_ref):
    total = qkv_ref.shape[1]
    width = qkv_ref.shape[2]
    heads = width // HEAD
    per = shift_ref.shape[2]
    scale = HEAD ** (-0.5)
    lane = lax.broadcasted_iota(jnp.int32, (TILE, width), 1) // HEAD
    strict = lax.broadcasted_iota(jnp.int32, (TILE, TILE), 1) < lax.broadcasted_iota(
        jnp.int32, (TILE, TILE), 0
    )
    tri = tri_ref[...]
    for i in range(total // TILE):
        q_all = qkv_ref[0, i * TILE : (i + 1) * TILE]
        result = jnp.zeros((TILE, width), jnp.float32)
        q_heads = [jnp.where(lane == h, q_all, jnp.zeros_like(q_all)) for h in range(heads)]
        running = [jnp.zeros((TILE, width), jnp.float32) for _ in range(heads)]
        logsum = [jnp.zeros((TILE, 1), jnp.float32) for _ in range(heads)]
        for j in range(i, -1, -1):
            k_all = qkv_ref[1, j * TILE : (j + 1) * TILE]
            v_all = qkv_ref[2, j * TILE : (j + 1) * TILE]
            for h in range(heads):
                shift = jnp.concatenate(
                    [
                        shift_ref[j * (TILE // per) + p, h : h + 1]
                        for p in range(TILE // per)
                    ],
                    axis=1,
                )
                score = (
                    lax.dot_general(
                        q_heads[h],
                        k_all,
                        (((1,), (1,)), ((), ())),
                        preferred_element_type=jnp.float32,
                    )
                    * scale
                    + shift
                )
                tail = jnp.log(1.0 + jnp.exp(-jnp.abs(score)))
                log_take = jnp.minimum(score, 0.0) - tail
                log_keep = -jnp.maximum(score, 0.0) - tail
                if i == j:
                    log_keep = jnp.where(strict, log_keep, 0.0)
                high = log_keep.astype(jnp.bfloat16)
                low = (log_keep - high.astype(jnp.float32)).astype(jnp.bfloat16)
                later = jnp.dot(high, tri, preferred_element_type=jnp.float32) + jnp.dot(
                    low, tri, preferred_element_type=jnp.float32
                )
                weight = jnp.exp(log_take + later + logsum[h])
                if i == j:
                    weight = jnp.where(strict, weight, 0.0)
                running[h] = running[h] + jnp.dot(
                    weight.astype(jnp.bfloat16), v_all, preferred_element_type=jnp.float32
                )
                logsum[h] = logsum[h] + later[:, :1] + log_keep[:, :1]
        for h in range(heads):
            result = jnp.where(lane == h, running[h], result)
        out_ref[i * TILE : (i + 1) * TILE] = result.astype(jnp.bfloat16)


def stick(qkv, shift_rows):
    position = jnp.arange(TILE, dtype=jnp.int32)
    tri = (position[:, None] > position[None, :]).astype(jnp.bfloat16)
    vmem_spec = pl.BlockSpec(memory_space=pltpu.VMEM)
    return pl.pallas_call(
        stick_kernel,
        out_shape=jax.ShapeDtypeStruct(qkv.shape[1:], jnp.bfloat16),
        in_specs=[vmem_spec] * 3,
        out_specs=vmem_spec,
    )(qkv, shift_rows, tri)


def regroup_kernel(ep_count, att_ref, out_ref, send, recv, own_sem):
    e = lax.axis_index("ep")
    t = lax.axis_index("tp")
    block = out_ref.shape[0]
    width = att_ref.shape[1]
    meet([((e + d) % ep_count, t) for d in range(1, ep_count)])
    cols = pl.ds(pl.multiple_of(e * width, width), width)
    copies = []
    for d in range(1, ep_count):
        to = (e + d) % ep_count
        part = pl.ds(pl.multiple_of(to * block, block), block)
        copies.append(
            push(att_ref.at[part], out_ref.at[:, cols], send.at[d - 1], recv.at[d - 1], to, t)
        )
    own = pltpu.make_async_copy(
        att_ref.at[pl.ds(pl.multiple_of(e * block, block), block)], out_ref.at[:, cols], own_sem
    )
    own.start()
    for copy in copies:
        copy.wait()
    own.wait()


def regroup(attended, ep_count):
    rows, width = attended.shape

    def kernel(*refs):
        regroup_kernel(ep_count, *refs)

    return pl.pallas_call(
        kernel,
        out_shape=jax.ShapeDtypeStruct((rows // ep_count, width * ep_count), jnp.bfloat16),
        in_specs=[pl.BlockSpec(memory_space=pltpu.VMEM)],
        out_specs=pl.BlockSpec(memory_space=pl.ANY),
        scratch_shapes=[
            pltpu.SemaphoreType.DMA((ep_count - 1,)),
            pltpu.SemaphoreType.DMA((ep_count - 1,)),
            pltpu.SemaphoreType.DMA,
        ],
        compiler_params=pltpu.CompilerParams(collective_id=1, has_side_effects=True),
    )(attended)


def collect_kernel(
    part_ref, proj_ref, mixed_ref, home_ref,
    got_c, got_o, pair, pair_o, got_x, got_y, mid_x, mid_y, got_x2, got_y2, got_oy, final,
    send, recv, recv_z,
):
    e = lax.axis_index("ep")
    t = lax.axis_index("tp")
    g = e // 2
    x = e % 2
    y = t // 2
    c = t % 2
    e_x = g * 2 + (1 - x)
    t_y = (t + 2) % 4
    t_c = t + 1 - 2 * c
    others = [((g + dz) % GROUPS * 2 + x, t) for dz in range(1, GROUPS)]
    meet(others + [(e_x, t), (e, t_y), (e, t_c)])
    half = GROUPS // 2
    copies = []

    def go(src, dst, ep_to, tp_to):
        n = len(copies)
        copy = push(src, dst, send.at[n], recv.at[n], ep_to, tp_to)
        copies.append(copy)
        return copy

    def add(a, b):
        return (a.astype(jnp.float32) + b.astype(jnp.float32)).astype(jnp.bfloat16)

    swaps = {}
    firsts = []
    for zi in range(half):
        for k in range(2):
            firsts.append(("x", zi, k))
            firsts.append(("y", zi, k))
    seconds = []
    for zi in range(half):
        for k in range(2):
            seconds.append(("x2", zi, k))
            seconds.append(("y2", zi, k))

    def spot(kind, zi, k):
        if kind == "x":
            return zi, 1 - x, k
        if kind == "y":
            return half + zi, k, 1 - y
        if kind == "x2":
            return zi, x, k
        return half + zi, k, y

    swap_o = [None, None]
    for item in firsts + seconds:
        z, xi, yi = spot(*item)
        swaps[item] = go(
            part_ref.at[z, xi, yi * 2 + 1 - c], got_c.at[z, xi, yi], e, t_c
        )
        if item == firsts[-1]:
            for k in range(2):
                yk = 1 - y if k == 0 else y
                swap_o[k] = go(proj_ref.at[yk * 2 + 1 - c], got_o.at[yk], e, t_c)
    hops = {}
    for item in firsts:
        kind, zi, k = item
        z, xi, yi = spot(*item)
        swaps[item].wait_recv()
        pair[z, xi, yi] = add(part_ref[z, xi, yi * 2 + c], got_c[z, xi, yi])
        if kind == "x":
            hops[item] = go(pair.at[z, xi, yi], got_x.at[zi, k], e_x, t)
        else:
            hops[item] = go(pair.at[z, xi, yi], got_y.at[zi, k], e, t_y)
    swap_o[0].wait_recv()
    pair_o[1 - y] = add(proj_ref[(1 - y) * 2 + c], got_o[1 - y])
    hop_o = go(pair_o.at[1 - y], got_oy, e, t_y)
    for item in seconds:
        z, xi, yi = spot(*item)
        swaps[item].wait_recv()
        pair[z, xi, yi] = add(part_ref[z, xi, yi * 2 + c], got_c[z, xi, yi])
    swap_o[1].wait_recv()
    pair_o[y] = add(proj_ref[y * 2 + c], got_o[y])
    last = []
    for zi in range(half):
        for k in range(2):
            hops[("x", zi, k)].wait_recv()
            mid_x[zi, k] = add(pair[zi, x, k], got_x[zi, k])
            hops[("y", zi, k)].wait_recv()
            mid_y[zi, k] = add(pair[half + zi, k, y], got_y[zi, k])
        last.append(
            (
                go(mid_x.at[zi, 1 - y], got_x2.at[zi], e, t_y),
                go(mid_y.at[zi, 1 - x], got_y2.at[zi], e_x, t),
            )
        )
    hop_o.wait_recv()
    mixed_ref[...] = add(pair_o[y], got_oy[...])
    for zi in range(half):
        last[zi][0].wait_recv()
        final[zi] = add(mid_x[zi, y], got_x2[zi])
        last[zi][1].wait_recv()
        final[half + zi] = add(mid_y[zi, x], got_y2[zi])
    backs = []
    for dz in range(1, GROUPS):
        to = (g + dz) % GROUPS
        copy = push(
            final.at[to], home_ref.at[g], send.at[len(copies) + dz - 1], recv_z.at[dz - 1],
            to * 2 + x, t,
        )
        backs.append(copy)
    home_ref[g] = final[g]
    for copy in copies:
        copy.wait_send()
    for copy in backs:
        copy.wait()


def collect(part, proj):
    _, _, tp_count, slots, model_width = part.shape
    sub = proj.shape[1]
    half = GROUPS // 2
    vmem_spec = pl.BlockSpec(memory_space=pltpu.VMEM)
    bf = jnp.bfloat16
    block = (slots, model_width)
    return pl.pallas_call(
        collect_kernel,
        out_shape=(
            jax.ShapeDtypeStruct((sub, model_width), bf),
            jax.ShapeDtypeStruct((GROUPS, *block), bf),
        ),
        in_specs=[vmem_spec] * 2,
        out_specs=(vmem_spec,) * 2,
        scratch_shapes=[
            pltpu.VMEM((GROUPS, 2, 2, *block), bf),
            pltpu.VMEM((2, sub, model_width), bf),
            pltpu.VMEM((GROUPS, 2, 2, *block), bf),
            pltpu.VMEM((2, sub, model_width), bf),
            pltpu.VMEM((half, 2, *block), bf),
            pltpu.VMEM((half, 2, *block), bf),
            pltpu.VMEM((half, 2, *block), bf),
            pltpu.VMEM((half, 2, *block), bf),
            pltpu.VMEM((half, *block), bf),
            pltpu.VMEM((half, *block), bf),
            pltpu.VMEM((sub, model_width), bf),
            pltpu.VMEM((GROUPS, *block), bf),
            pltpu.SemaphoreType.DMA((40,)),
            pltpu.SemaphoreType.DMA((40,)),
            pltpu.SemaphoreType.DMA((GROUPS - 1,)),
        ],
        compiler_params=pltpu.CompilerParams(
            collective_id=2, has_side_effects=True, vmem_limit_bytes=60000 * 1024
        ),
    )(part, proj)


def shards_paired(
    queries, key_rows, value_rows, key_shift, out_weight, routed_rows, expert_ids,
    route_weights, gate_weight, up_weight, down_weight,
):
    ep_count = lax.axis_size("ep")
    tp_count = lax.axis_size("tp")
    local_rows = queries.shape[0]
    sub = local_rows // tp_count
    slots = 4 * sub // ep_count
    model_width = routed_rows.shape[1]
    column = lax.axis_index("tp")
    x = lax.axis_index("ep") % 2

    ids = lax.dynamic_slice_in_dim(expert_ids, column * sub, sub, 0)
    own_rows = lax.dynamic_slice_in_dim(routed_rows, column * sub, sub, 0)
    group = ids[:, 0] // 2
    token = jnp.arange(sub, dtype=jnp.int32)
    earlier = (group[:, None] == group[None, :]) & (token[None, :] < token[:, None])
    place = group * slots + jnp.sum(earlier.astype(jnp.int32), axis=1)
    pick = place[None, :] == jnp.arange(GROUPS * slots, dtype=jnp.int32)[:, None]
    packed = jnp.dot(pick.astype(jnp.bfloat16), own_rows, preferred_element_type=jnp.float32)
    side = [
        jnp.sum(jnp.where(ids % 2 == s, route_weights, 0.0), axis=1) for s in range(2)
    ]
    pieces = []
    for weights in side:
        spread_w = jnp.sum(jnp.where(pick, weights[None, :], 0.0), axis=1)
        first = lax.reduce_precision(spread_w, 8, 7)
        second = lax.reduce_precision(spread_w - first, 8, 7)
        pieces += [first, second, spread_w - first - second]
    extra = jnp.pad(jnp.stack(pieces, axis=1), ((0, 0), (0, 128 - len(pieces))))
    rows = jnp.concatenate([packed.astype(jnp.bfloat16), extra.astype(jnp.bfloat16)], axis=1)
    rows = rows.reshape(GROUPS, slots, model_width + 128)

    per = key_shift.shape[1] // ep_count
    shift_rows = key_shift.astype(jnp.float32).T.reshape(ep_count, per, local_rows)
    shift_rows = jnp.pad(shift_rows, ((0, 0), (0, -per % 8), (0, 0)))
    qkv, shift_all, gathered = spread(
        queries, key_rows, value_rows, shift_rows, rows, ep_count, tp_count
    )
    attended = regroup(stick(qkv, shift_all), ep_count)
    proj = jnp.dot(attended, out_weight, preferred_element_type=jnp.float32).astype(jnp.bfloat16)

    gathered = gathered.reshape(-1, model_width + 128)
    expert_rows = gathered[:, :model_width]
    marks = lax.dynamic_slice_in_dim(gathered[:, model_width:], 3 * x, 3, 1).astype(jnp.float32)
    scale = marks[:, 0:1] + marks[:, 1:2] + marks[:, 2:3]
    gate = jnp.dot(expert_rows, gate_weight[0], preferred_element_type=jnp.float32)
    up = jnp.dot(expert_rows, up_weight[0], preferred_element_type=jnp.float32)
    hidden = (jax.nn.silu(gate) * up).astype(jnp.bfloat16)
    part = jnp.dot(hidden, down_weight[0], preferred_element_type=jnp.float32)
    part = (part * scale).astype(jnp.bfloat16)
    mixed_rows, home = collect(
        part.reshape(GROUPS, 2, tp_count, slots, model_width),
        proj.reshape(tp_count, sub, model_width),
    )
    home = home.reshape(GROUPS * slots, model_width)
    routed_out = jnp.dot(
        pick.T.astype(jnp.bfloat16), home, preferred_element_type=jnp.float32
    ).astype(jnp.bfloat16)
    return (mixed_rows, routed_out)


def shards(
    queries,
    key_rows,
    value_rows,
    key_shift,
    out_weight,
    routed_rows,
    expert_ids,
    route_weights,
    gate_weight,
    up_weight,
    down_weight,
):
    tp_count = lax.axis_size("tp")
    local_rows = queries.shape[0]
    heads_here = key_shift.shape[1]
    key_all, value_all, shift_all = (
        lax.all_gather(key_rows, "ep", axis=0, tiled=True),
        lax.all_gather(value_rows, "ep", axis=0, tiled=True),
        lax.all_gather(key_shift, "ep", axis=0, tiled=True),
    )
    first_pos = lax.axis_index("ep") * local_rows
    attended = stick_attend(
        queries.reshape(local_rows, heads_here, HEAD), key_all, value_all, shift_all, first_pos
    )
    mixed_rows = lax.psum_scatter(
        jnp.dot(attended, out_weight, preferred_element_type=jnp.float32).astype(jnp.bfloat16),
        "tp",
        scatter_dimension=0,
        tiled=True,
    )
    expert_count = lax.axis_size("ep")
    sub_rows = local_rows // tp_count
    capacity = 4 * sub_rows // expert_count
    model_width = routed_rows.shape[1]
    column = lax.axis_index("tp")
    own_ids = lax.dynamic_slice_in_dim(expert_ids, column * sub_rows, sub_rows, 0).reshape(
        1, sub_rows * 2
    )
    own_slot = slot_numbers(own_ids, expert_count)[0]
    own_dest = own_ids[0] * capacity + own_slot
    own_input = lax.dynamic_slice_in_dim(routed_rows, column * sub_rows, sub_rows, 0)
    outgoing = pack_rows(own_input, own_dest, expert_count * capacity).reshape(
        expert_count, capacity, model_width
    )
    arrived = lax.all_to_all(outgoing, "ep", split_axis=0, concat_axis=0, tiled=True)
    hidden = expand(lax.all_gather(arrived, "tp", axis=1, tiled=True), gate_weight[0], up_weight[0])
    unit_count = hidden.shape[2]
    ordered = jnp.transpose(
        hidden.reshape(expert_count, tp_count, capacity, unit_count), (1, 0, 2, 3)
    )
    ordered = ordered.reshape(tp_count * expert_count * capacity, unit_count)
    partial_value = lax.psum_scatter(
        jnp.dot(ordered, down_weight[0], preferred_element_type=jnp.float32).astype(jnp.bfloat16),
        "tp",
        scatter_dimension=0,
        tiled=True,
    )
    returned = lax.all_to_all(
        partial_value.reshape(expert_count, capacity, model_width),
        "ep",
        split_axis=0,
        concat_axis=0,
        tiled=True,
    )
    picked = jnp.take(returned.reshape(expert_count * capacity, model_width), own_dest, axis=0)
    picked = picked.reshape(sub_rows, 2, model_width).astype(jnp.float32)
    routed_out = (
        picked[:, 0] * route_weights[:, 0:1] + picked[:, 1] * route_weights[:, 1:2]
    ).astype(jnp.bfloat16)
    return (mixed_rows, routed_out)


def solution(mesh):
    paired = mesh.shape["ep"] == 2 * GROUPS and mesh.shape["tp"] == 4
    return jax.shard_map(
        shards_paired if paired else shards,
        mesh=mesh,
        in_specs=(
            P("ep", "tp"),
            P("ep", "tp"),
            P("ep", "tp"),
            P("ep", "tp"),
            P("tp", None),
            P("ep", None),
            P("ep", None),
            P(("ep", "tp"), None),
            P("ep", None, "tp"),
            P("ep", None, "tp"),
            P("ep", "tp", None),
        ),
        out_specs=(P(("ep", "tp"), None), P(("ep", "tp"), None)),
        check_vma=False,
    )
```

```python
import jax
import jax.numpy as jnp
from jax import lax
from jax.experimental import pallas as pl
from jax.experimental.pallas import tpu as pltpu
from jax.sharding import PartitionSpec as P

HEAD = 64
KEY_BLOCK = 512
GROUPS = 4
TILE = 256
MESH = pl.DeviceIdType.MESH


def stick_attend(query_rows, key_all, value_all, shift_all, first_pos):
    row_count = query_rows.shape[0]
    head_count = query_rows.shape[1]
    head_depth = query_rows.shape[2]
    query_pos = first_pos + jnp.arange(row_count, dtype=jnp.int32)
    last_block = (first_pos + row_count - 1) // KEY_BLOCK
    score_scale = head_depth ** (-0.5)

    def sweep_block(step_index, state_pair):
        running, logsum = state_pair
        row_start = (last_block - step_index) * KEY_BLOCK
        key_tile_block = lax.dynamic_slice_in_dim(key_all, row_start, KEY_BLOCK, 0).reshape(
            KEY_BLOCK, head_count, head_depth
        )
        value_block = lax.dynamic_slice_in_dim(value_all, row_start, KEY_BLOCK, 0).reshape(
            KEY_BLOCK, head_count, head_depth
        )
        shift_block = lax.dynamic_slice_in_dim(shift_all, row_start, KEY_BLOCK, 0).astype(
            jnp.float32
        )
        scores = (
            jnp.einsum(
                "thd,shd->hts", query_rows, key_tile_block, preferred_element_type=jnp.float32
            )
            * score_scale
        )
        scores = scores + shift_block.T[:, None, :]
        key_pos = row_start + jnp.arange(KEY_BLOCK, dtype=jnp.int32)
        strict = (key_pos[None, :] < query_pos[:, None])[None]
        log_keep = jnp.where(strict, jax.nn.log_sigmoid(-scores), 0.0)
        suffix = lax.cumsum(log_keep, axis=2, reverse=True) - log_keep + logsum[:, :, None]
        weight = jnp.where(strict, jnp.exp(jax.nn.log_sigmoid(scores) + suffix), 0.0).astype(
            jnp.bfloat16
        )
        running = running + jnp.einsum(
            "hts,shd->htd", weight, value_block, preferred_element_type=jnp.float32
        )
        return (running, logsum + jnp.sum(log_keep, axis=2))

    initial = (
        jnp.zeros((head_count, row_count, head_depth), jnp.float32),
        jnp.zeros((head_count, row_count), jnp.float32),
    )
    running, logsum = lax.fori_loop(0, last_block + 1, sweep_block, initial)
    return (
        jnp.transpose(running, (1, 0, 2))
        .reshape(row_count, head_count * head_depth)
        .astype(jnp.bfloat16)
    )


def slot_numbers(pair_ids, expert_count):
    one_hot = (pair_ids[..., None] == jnp.arange(expert_count, dtype=jnp.int32)).astype(jnp.int32)
    earlier = jnp.cumsum(one_hot, axis=1) - one_hot
    return jnp.sum(one_hot * earlier, axis=2)


def pack_rows(source_rows, destination, slot_count):
    pair_count = destination.shape[0]
    matches = destination[None, :] == jnp.arange(slot_count, dtype=jnp.int32)[:, None]
    source_index = jnp.sum(
        jnp.where(matches, jnp.arange(pair_count, dtype=jnp.int32)[None, :] // 2, 0), axis=1
    )
    filled = jnp.any(matches, axis=1)
    picked = jnp.take(source_rows, source_index, axis=0)
    return jnp.where(filled[:, None], picked, jnp.zeros_like(picked))


def expand(expert_rows, gate_part, up_part):
    gate_proj = jnp.einsum(
        "rcd,df->rcf", expert_rows, gate_part, preferred_element_type=jnp.float32
    )
    up_proj = jnp.einsum("rcd,df->rcf", expert_rows, up_part, preferred_element_type=jnp.float32)
    return (jax.nn.silu(gate_proj) * up_proj).astype(jnp.bfloat16)


def meet(devices):
    barrier = pltpu.get_barrier_semaphore()
    for ep_to, tp_to in devices:
        pl.semaphore_signal(
            barrier, inc=1, device_id={"ep": ep_to, "tp": tp_to}, device_id_type=MESH
        )
    pl.semaphore_wait(barrier, len(devices))


def push(src, dst, send, recv, ep_to, tp_to):
    copy = pltpu.make_async_remote_copy(
        src_ref=src,
        dst_ref=dst,
        send_sem=send,
        recv_sem=recv,
        device_id={"ep": ep_to, "tp": tp_to},
        device_id_type=MESH,
    )
    copy.start()
    return copy


def fused_kernel(
    ep_count,
    q_ref, k_ref, v_ref, s_ref, rows_ref, tri_ref, ow_hbm, gw_hbm, uw_hbm, dw_hbm,
    mixed_ref, home_ref,
    ow, gw, uw, dw, qkv, shifts, gath, part, got_c, pair, got1, mid, got2, final,
    att, att_all, proj, got_o, pair_o, got_oy,
    send_a, recv_a, send_b, recv_b, send_r, recv_r, send_s, recv_s, own_sem, load_sem,
):
    e = lax.axis_index("ep")
    t = lax.axis_index("tp")
    g = e // 2
    x = e % 2
    y = t // 2
    c = t % 2
    e_x = g * 2 + (1 - x)
    t_y = (t + 2) % 4
    t_c = t + 1 - 2 * c
    t_yc = (t_c + 2) % 4
    block = q_ref.shape[0]
    width = q_ref.shape[1] // ep_count
    slots = rows_ref.shape[1]
    model = mixed_ref.shape[1]
    order = (0, 3, 1, 2)
    x_first = (0, 1)

    loads = []
    for n, (src, dst) in enumerate(((gw_hbm, gw), (uw_hbm, uw), (dw_hbm, dw), (ow_hbm, ow))):
        load = pltpu.make_async_copy(src, dst, load_sem.at[n])
        load.start()
        loads.append(load)
    owns = []

    def keep(src, dst):
        own = pltpu.make_async_copy(src, dst, own_sem.at[len(owns)])
        own.start()
        owns.append(own)
        return own

    mine = pl.ds(pl.multiple_of(e * width, width), width)
    here = pl.ds(pl.multiple_of(e * block, block), block)
    kept_rows = keep(rows_ref.at[g], gath.at[g, x, t])
    for i, ref in enumerate((q_ref, k_ref, v_ref)):
        keep(ref.at[:, mine], qkv.at[i, here])
    keep(s_ref.at[e], shifts.at[e])
    meet([((e + d) % ep_count, t) for d in range(1, ep_count)] + [(e, t_y), (e, t_c)])

    sends = []

    def send_rows(src, z, xi, ti, ep_to, tp_to):
        sends.append(
            push(
                src, gath.at[z, xi, ti], send_b.at[len(sends)], recv_b.at[z, xi, ti], ep_to, tp_to
            )
        )

    def forward(z, xi, ti, ep_to, tp_to):
        send_rows(gath.at[z, xi, ti], z, xi, ti, ep_to, tp_to)

    def arrived(z, xi, ti):
        place = gath.at[z, xi, ti]
        pltpu.make_async_copy(place, place, recv_b.at[z, xi, ti]).wait()

    for dz in (3, 1, 2):
        to = (g + dz) % GROUPS
        send_rows(rows_ref.at[to], g, x, t, to * 2 + x, t)
    for ep_to, tp_to in ((e_x, t), (e, t_y), (e, t_c)):
        send_rows(rows_ref.at[g], g, x, t, ep_to, tp_to)
    exchange = []
    for d in range(1, ep_count):
        to = (e + d) % ep_count
        cols = pl.ds(pl.multiple_of(to * width, width), width)
        for i, ref in enumerate((q_ref, k_ref, v_ref)):
            exchange.append(
                push(
                    ref.at[:, cols], qkv.at[i, here],
                    send_a.at[i, d - 1], recv_a.at[i, d - 1], to, t,
                )
            )
        exchange.append(
            push(s_ref.at[to], shifts.at[e], send_a.at[3, d - 1], recv_a.at[3, d - 1], to, t)
        )

    later_sends = []

    def go(src, dst, ep_to, tp_to):
        n = len(later_sends)
        copy = push(src, dst, send_s.at[n], recv_s.at[n], ep_to, tp_to)
        later_sends.append(copy)
        return copy

    def add(a, b):
        return (a.astype(jnp.float32) + b.astype(jnp.float32)).astype(jnp.bfloat16)

    def plane_of(dz):
        return (g + dz) % GROUPS

    def first_leg(dz):
        z = plane_of(dz)
        arrived(z, x, t)
        forward(z, x, t, e_x, t)
        forward(z, x, t, e, t_y)
        forward(z, x, t, e, t_c)

    def second_leg(dz):
        z = plane_of(dz)
        arrived(z, 1 - x, t)
        if dz in (0, 3):
            forward(z, 1 - x, t, e, t_y)
        forward(z, 1 - x, t, e, t_c)
        arrived(z, x, t_y)
        if dz not in (0, 3):
            forward(z, x, t_y, e_x, t)
        forward(z, x, t_y, e, t_c)

    def third_leg(dz):
        z = plane_of(dz)
        arrived(z, 1 - x, t_y)
        forward(z, 1 - x, t_y, e, t_c)

    lane = lax.broadcasted_iota(jnp.int32, (2 * 4 * slots, rows_ref.shape[2] - model), 1)
    chosen = (lane >= 3 * x) & (lane < 3 * x + 3)
    swaps = {}
    hops = {}
    ends = {}

    def experts(dz):
        z = plane_of(dz)
        for xi in (x, 1 - x):
            arrived(z, xi, t_c)
            arrived(z, xi, t_yc)
        rows = gath[z].reshape(2 * 4 * slots, rows_ref.shape[2])
        inputs = rows[:, :model]
        marks = rows[:, model:].astype(jnp.float32)
        scale = jnp.sum(jnp.where(chosen, marks, 0.0), axis=1, keepdims=True)
        gate = jnp.dot(inputs, gw[...], preferred_element_type=jnp.float32)
        up = jnp.dot(inputs, uw[...], preferred_element_type=jnp.float32)
        hidden = (gate / (1.0 + jnp.exp(-gate)) * up).astype(jnp.bfloat16)
        step = model // 4
        for n in range(4):
            cols = slice(n * step, (n + 1) * step)
            down = jnp.dot(hidden, dw[:, cols], preferred_element_type=jnp.float32)
            down = (down * scale).astype(jnp.bfloat16)
            for xi in range(2):
                for ti in range(4):
                    at = (xi * 4 + ti) * slots
                    part[dz, ti % 2, xi, ti // 2, :, cols] = down[at : at + slots]
        swaps[dz] = go(part.at[dz, 1 - c], got_c.at[dz], e, t_c)

    def pair_sum(dz):
        swaps[dz].wait_recv()
        pair[dz] = add(part[dz, c], got_c[dz])
        if dz in x_first:
            hops[dz] = go(pair.at[dz, 1 - x], got1.at[dz], e_x, t)
        else:
            hops[dz] = go(pair.at[dz, :, 1 - y], got1.at[dz], e, t_y)

    def middle_sum(dz):
        hops[dz].wait_recv()
        if dz in x_first:
            mid[dz] = add(pair[dz, x], got1[dz])
            ends[dz] = go(mid.at[dz, 1 - y], got2.at[dz], e, t_y)
        else:
            mid[dz] = add(pair[dz, :, y], got1[dz])
            ends[dz] = go(mid.at[dz, 1 - x], got2.at[dz], e_x, t)

    backs = []

    def send_home(dz):
        ends[dz].wait_recv()
        total = add(mid[dz, y if dz in x_first else x], got2[dz])
        if dz == 0:
            home_ref[g] = total
        else:
            final[dz] = total
            backs.append(go(final.at[dz], home_ref.at[g], plane_of(dz) * 2 + x, t))

    kept_rows.wait()
    second_leg(0)
    first_leg(3)
    first_leg(1)
    second_leg(3)
    third_leg(0)
    first_leg(2)
    second_leg(1)
    third_leg(3)
    for load in loads[:3]:
        load.wait()
    experts(0)
    second_leg(2)
    third_leg(1)
    experts(3)
    third_leg(2)
    pair_sum(0)
    experts(1)
    pair_sum(3)
    experts(2)
    pair_sum(1)
    pair_sum(2)
    for copy in exchange:
        copy.wait()
    for own in owns[1:]:
        own.wait()
    tri = tri_ref[...]
    middle_sum(0)
    middle_sum(3)
    blocks = att.shape[0] // TILE
    stick_block(blocks - 1, qkv, shifts, tri, att)
    middle_sum(1)
    middle_sum(2)
    for i in range(blocks - 2, -1, -1):
        stick_block(i, qkv, shifts, tri, att)
    regroups = []
    for d in range(1, ep_count):
        to = (e + d) % ep_count
        rows = pl.ds(pl.multiple_of(to * block, block), block)
        regroups.append(
            push(
                att.at[rows], att_all.at[:, mine], send_r.at[d - 1], recv_r.at[d - 1], to, t
            )
        )
    own_heads = keep(att.at[here], att_all.at[:, mine])
    for dz in (3, 1, 2, 0):
        send_home(dz)
    for copy in regroups:
        copy.wait()
    own_heads.wait()
    loads[3].wait()
    sub = mixed_ref.shape[0]
    chunk = 512

    def project(n, carry):
        cols = pl.ds(pl.multiple_of(n * chunk, chunk), chunk)
        value = jnp.dot(att_all[...], ow[:, cols], preferred_element_type=jnp.float32)
        value = value.astype(jnp.bfloat16)
        for ti in range(4):
            proj[ti % 2, ti // 2, :, cols] = value[ti * sub : (ti + 1) * sub]
        return carry

    lax.fori_loop(0, model // chunk, project, 0)
    swap_o = go(proj.at[1 - c], got_o, e, t_c)
    swap_o.wait_recv()
    pair_o[1 - y] = add(proj[c, 1 - y], got_o[1 - y])
    hop_o = go(pair_o.at[1 - y], got_oy, e, t_y)
    pair_o[y] = add(proj[c, y], got_o[y])
    hop_o.wait_recv()
    mixed_ref[...] = add(pair_o[y], got_oy[...])
    for copy in backs:
        copy.wait_recv()
    for copy in sends + later_sends:
        copy.wait_send()


def stick_block(i, qkv, shifts, tri, out_ref):
    width = qkv.shape[2]
    heads = width // HEAD
    per = shifts.shape[2]
    score_scale = HEAD ** (-0.5)
    lane = lax.broadcasted_iota(jnp.int32, (TILE, width), 1) // HEAD
    strict = lax.broadcasted_iota(jnp.int32, (TILE, TILE), 1) < lax.broadcasted_iota(
        jnp.int32, (TILE, TILE), 0
    )
    q_all = qkv[0, i * TILE : (i + 1) * TILE]
    q_heads = [jnp.where(lane == h, q_all, jnp.zeros_like(q_all)) for h in range(heads)]
    running = [jnp.zeros((TILE, width), jnp.float32) for _ in range(heads)]
    logsum = [jnp.zeros((TILE, 1), jnp.float32) for _ in range(heads)]
    for j in range(i, -1, -1):
        k_all = qkv[1, j * TILE : (j + 1) * TILE]
        v_all = qkv[2, j * TILE : (j + 1) * TILE]
        for h in range(heads):
            shift = jnp.concatenate(
                [shifts[j * (TILE // per) + p, h : h + 1] for p in range(TILE // per)], axis=1
            )
            score = (
                lax.dot_general(
                    q_heads[h],
                    k_all,
                    (((1,), (1,)), ((), ())),
                    preferred_element_type=jnp.float32,
                )
                * score_scale
                + shift
            )
            tail = jnp.log(1.0 + jnp.exp(-jnp.abs(score)))
            log_take = jnp.minimum(score, 0.0) - tail
            log_keep = -jnp.maximum(score, 0.0) - tail
            if i == j:
                log_keep = jnp.where(strict, log_keep, 0.0)
            high = log_keep.astype(jnp.bfloat16)
            low = (log_keep - high.astype(jnp.float32)).astype(jnp.bfloat16)
            later = jnp.dot(high, tri, preferred_element_type=jnp.float32) + jnp.dot(
                low, tri, preferred_element_type=jnp.float32
            )
            weight = jnp.exp(log_take + later + logsum[h])
            if i == j:
                weight = jnp.where(strict, weight, 0.0)
            running[h] = running[h] + jnp.dot(
                weight.astype(jnp.bfloat16), v_all, preferred_element_type=jnp.float32
            )
            logsum[h] = logsum[h] + later[:, :1] + log_keep[:, :1]
    result = running[0]
    for h in range(1, heads):
        result = jnp.where(lane == h, running[h], result)
    out_ref[i * TILE : (i + 1) * TILE] = result.astype(jnp.bfloat16)


def fused(q, k, v, shift_rows, rows, out_w, gate_w, up_w, down_w, ep_count, tp_count):
    block = q.shape[0]
    width = q.shape[1] // ep_count
    slots, row_width = rows.shape[1:]
    model = out_w.shape[1]
    sub = block // tp_count
    position = jnp.arange(TILE, dtype=jnp.int32)
    tri = (position[:, None] > position[None, :]).astype(jnp.bfloat16)
    vmem_spec = pl.BlockSpec(memory_space=pltpu.VMEM)
    any_spec = pl.BlockSpec(memory_space=pl.ANY)
    bf = jnp.bfloat16
    dma = pltpu.SemaphoreType.DMA
    one = (slots, model)

    def kernel(*refs):
        fused_kernel(ep_count, *refs)

    return pl.pallas_call(
        kernel,
        out_shape=(
            jax.ShapeDtypeStruct((sub, model), bf),
            jax.ShapeDtypeStruct((GROUPS, *one), bf),
        ),
        in_specs=[vmem_spec] * 6 + [any_spec] * 4,
        out_specs=(vmem_spec,) * 2,
        scratch_shapes=[
            pltpu.VMEM(out_w.shape, bf),
            pltpu.VMEM(gate_w.shape, bf),
            pltpu.VMEM(up_w.shape, bf),
            pltpu.VMEM(down_w.shape, bf),
            pltpu.VMEM((3, block * ep_count, width), bf),
            pltpu.VMEM(shift_rows.shape, jnp.float32),
            pltpu.VMEM((GROUPS, 2, tp_count, slots, row_width), bf),
            pltpu.VMEM((GROUPS, 2, 2, 2, *one), bf),
            pltpu.VMEM((GROUPS, 2, 2, *one), bf),
            pltpu.VMEM((GROUPS, 2, 2, *one), bf),
            pltpu.VMEM((GROUPS, 2, *one), bf),
            pltpu.VMEM((GROUPS, 2, *one), bf),
            pltpu.VMEM((GROUPS, *one), bf),
            pltpu.VMEM((GROUPS, *one), bf),
            pltpu.VMEM((block * ep_count, width), bf),
            pltpu.VMEM(q.shape, bf),
            pltpu.VMEM((2, 2, sub, model), bf),
            pltpu.VMEM((2, sub, model), bf),
            pltpu.VMEM((2, sub, model), bf),
            pltpu.VMEM((sub, model), bf),
            dma((4, ep_count - 1)),
            dma((4, ep_count - 1)),
            dma((31,)),
            dma((GROUPS, 2, tp_count)),
            dma((ep_count - 1,)),
            dma((ep_count - 1,)),
            dma((17,)),
            dma((17,)),
            dma((6,)),
            dma((4,)),
        ],
        compiler_params=pltpu.CompilerParams(
            collective_id=0, has_side_effects=True, vmem_limit_bytes=60000 * 1024
        ),
    )(q, k, v, shift_rows, rows, tri, out_w, gate_w, up_w, down_w)


def shards_paired(
    queries, key_rows, value_rows, key_shift, out_weight, routed_rows, expert_ids,
    route_weights, gate_weight, up_weight, down_weight,
):
    ep_count = lax.axis_size("ep")
    tp_count = lax.axis_size("tp")
    local_rows = queries.shape[0]
    sub = local_rows // tp_count
    slots = 4 * sub // ep_count
    model_width = routed_rows.shape[1]
    column = lax.axis_index("tp")

    ids = lax.dynamic_slice_in_dim(expert_ids, column * sub, sub, 0)
    own_rows = lax.dynamic_slice_in_dim(routed_rows, column * sub, sub, 0)
    group = ids[:, 0] // 2
    token = jnp.arange(sub, dtype=jnp.int32)
    earlier = (group[:, None] == group[None, :]) & (token[None, :] < token[:, None])
    place = group * slots + jnp.sum(earlier.astype(jnp.int32), axis=1)
    pick = place[None, :] == jnp.arange(GROUPS * slots, dtype=jnp.int32)[:, None]
    packed = jnp.dot(pick.astype(jnp.bfloat16), own_rows, preferred_element_type=jnp.float32)
    side = [
        jnp.sum(jnp.where(ids % 2 == s, route_weights, 0.0), axis=1) for s in range(2)
    ]
    pieces = []
    for weights in side:
        spread_w = jnp.sum(jnp.where(pick, weights[None, :], 0.0), axis=1)
        first = lax.reduce_precision(spread_w, 8, 7)
        second = lax.reduce_precision(spread_w - first, 8, 7)
        pieces += [first, second, spread_w - first - second]
    extra = jnp.pad(jnp.stack(pieces, axis=1), ((0, 0), (0, 128 - len(pieces))))
    rows = jnp.concatenate([packed.astype(jnp.bfloat16), extra.astype(jnp.bfloat16)], axis=1)
    rows = rows.reshape(GROUPS, slots, model_width + 128)

    per = key_shift.shape[1] // ep_count
    shift_rows = key_shift.astype(jnp.float32).T.reshape(ep_count, per, local_rows)
    shift_rows = jnp.pad(shift_rows, ((0, 0), (0, -per % 8), (0, 0)))
    mixed_rows, home = fused(
        queries, key_rows, value_rows, shift_rows, rows,
        out_weight, gate_weight[0], up_weight[0], down_weight[0], ep_count, tp_count,
    )
    home = home.reshape(GROUPS * slots, model_width)
    routed_out = jnp.dot(
        pick.T.astype(jnp.bfloat16), home, preferred_element_type=jnp.float32
    ).astype(jnp.bfloat16)
    return (mixed_rows, routed_out)


def shards(
    queries,
    key_rows,
    value_rows,
    key_shift,
    out_weight,
    routed_rows,
    expert_ids,
    route_weights,
    gate_weight,
    up_weight,
    down_weight,
):
    tp_count = lax.axis_size("tp")
    local_rows = queries.shape[0]
    heads_here = key_shift.shape[1]
    key_all, value_all, shift_all = (
        lax.all_gather(key_rows, "ep", axis=0, tiled=True),
        lax.all_gather(value_rows, "ep", axis=0, tiled=True),
        lax.all_gather(key_shift, "ep", axis=0, tiled=True),
    )
    first_pos = lax.axis_index("ep") * local_rows
    attended = stick_attend(
        queries.reshape(local_rows, heads_here, HEAD), key_all, value_all, shift_all, first_pos
    )
    mixed_rows = lax.psum_scatter(
        jnp.dot(attended, out_weight, preferred_element_type=jnp.float32).astype(jnp.bfloat16),
        "tp",
        scatter_dimension=0,
        tiled=True,
    )
    expert_count = lax.axis_size("ep")
    sub_rows = local_rows // tp_count
    capacity = 4 * sub_rows // expert_count
    model_width = routed_rows.shape[1]
    column = lax.axis_index("tp")
    own_ids = lax.dynamic_slice_in_dim(expert_ids, column * sub_rows, sub_rows, 0).reshape(
        1, sub_rows * 2
    )
    own_slot = slot_numbers(own_ids, expert_count)[0]
    own_dest = own_ids[0] * capacity + own_slot
    own_input = lax.dynamic_slice_in_dim(routed_rows, column * sub_rows, sub_rows, 0)
    outgoing = pack_rows(own_input, own_dest, expert_count * capacity).reshape(
        expert_count, capacity, model_width
    )
    arrived = lax.all_to_all(outgoing, "ep", split_axis=0, concat_axis=0, tiled=True)
    hidden = expand(lax.all_gather(arrived, "tp", axis=1, tiled=True), gate_weight[0], up_weight[0])
    unit_count = hidden.shape[2]
    ordered = jnp.transpose(
        hidden.reshape(expert_count, tp_count, capacity, unit_count), (1, 0, 2, 3)
    )
    ordered = ordered.reshape(tp_count * expert_count * capacity, unit_count)
    partial_value = lax.psum_scatter(
        jnp.dot(ordered, down_weight[0], preferred_element_type=jnp.float32).astype(jnp.bfloat16),
        "tp",
        scatter_dimension=0,
        tiled=True,
    )
    returned = lax.all_to_all(
        partial_value.reshape(expert_count, capacity, model_width),
        "ep",
        split_axis=0,
        concat_axis=0,
        tiled=True,
    )
    picked = jnp.take(returned.reshape(expert_count * capacity, model_width), own_dest, axis=0)
    picked = picked.reshape(sub_rows, 2, model_width).astype(jnp.float32)
    routed_out = (
        picked[:, 0] * route_weights[:, 0:1] + picked[:, 1] * route_weights[:, 1:2]
    ).astype(jnp.bfloat16)
    return (mixed_rows, routed_out)


def solution(mesh):
    paired = mesh.shape["ep"] == 2 * GROUPS and mesh.shape["tp"] == 4
    return jax.shard_map(
        shards_paired if paired else shards,
        mesh=mesh,
        in_specs=(
            P("ep", "tp"),
            P("ep", "tp"),
            P("ep", "tp"),
            P("ep", "tp"),
            P("tp", None),
            P("ep", None),
            P("ep", None),
            P(("ep", "tp"), None),
            P("ep", None, "tp"),
            P("ep", None, "tp"),
            P("ep", "tp", None),
        ),
        out_specs=(P(("ep", "tp"), None), P(("ep", "tp"), None)),
        check_vma=False,
    )
```

```python
import jax
import jax.numpy as jnp
from jax import lax
from jax.experimental import pallas as pl
from jax.experimental.pallas import tpu as pltpu
from jax.sharding import PartitionSpec as P

HEAD = 64
KEY_BLOCK = 512
GROUPS = 4
TILE = 256
MESH = pl.DeviceIdType.MESH


def stick_attend(query_rows, key_all, value_all, shift_all, first_pos):
    row_count = query_rows.shape[0]
    head_count = query_rows.shape[1]
    head_depth = query_rows.shape[2]
    query_pos = first_pos + jnp.arange(row_count, dtype=jnp.int32)
    last_block = (first_pos + row_count - 1) // KEY_BLOCK
    score_scale = head_depth ** (-0.5)

    def sweep_block(step_index, state_pair):
        running, logsum = state_pair
        row_start = (last_block - step_index) * KEY_BLOCK
        key_tile_block = lax.dynamic_slice_in_dim(key_all, row_start, KEY_BLOCK, 0).reshape(
            KEY_BLOCK, head_count, head_depth
        )
        value_block = lax.dynamic_slice_in_dim(value_all, row_start, KEY_BLOCK, 0).reshape(
            KEY_BLOCK, head_count, head_depth
        )
        shift_block = lax.dynamic_slice_in_dim(shift_all, row_start, KEY_BLOCK, 0).astype(
            jnp.float32
        )
        scores = (
            jnp.einsum(
                "thd,shd->hts", query_rows, key_tile_block, preferred_element_type=jnp.float32
            )
            * score_scale
        )
        scores = scores + shift_block.T[:, None, :]
        key_pos = row_start + jnp.arange(KEY_BLOCK, dtype=jnp.int32)
        strict = (key_pos[None, :] < query_pos[:, None])[None]
        log_keep = jnp.where(strict, jax.nn.log_sigmoid(-scores), 0.0)
        suffix = lax.cumsum(log_keep, axis=2, reverse=True) - log_keep + logsum[:, :, None]
        weight = jnp.where(strict, jnp.exp(jax.nn.log_sigmoid(scores) + suffix), 0.0).astype(
            jnp.bfloat16
        )
        running = running + jnp.einsum(
            "hts,shd->htd", weight, value_block, preferred_element_type=jnp.float32
        )
        return (running, logsum + jnp.sum(log_keep, axis=2))

    initial = (
        jnp.zeros((head_count, row_count, head_depth), jnp.float32),
        jnp.zeros((head_count, row_count), jnp.float32),
    )
    running, logsum = lax.fori_loop(0, last_block + 1, sweep_block, initial)
    return (
        jnp.transpose(running, (1, 0, 2))
        .reshape(row_count, head_count * head_depth)
        .astype(jnp.bfloat16)
    )


def slot_numbers(pair_ids, expert_count):
    one_hot = (pair_ids[..., None] == jnp.arange(expert_count, dtype=jnp.int32)).astype(jnp.int32)
    earlier = jnp.cumsum(one_hot, axis=1) - one_hot
    return jnp.sum(one_hot * earlier, axis=2)


def pack_rows(source_rows, destination, slot_count):
    pair_count = destination.shape[0]
    matches = destination[None, :] == jnp.arange(slot_count, dtype=jnp.int32)[:, None]
    source_index = jnp.sum(
        jnp.where(matches, jnp.arange(pair_count, dtype=jnp.int32)[None, :] // 2, 0), axis=1
    )
    filled = jnp.any(matches, axis=1)
    picked = jnp.take(source_rows, source_index, axis=0)
    return jnp.where(filled[:, None], picked, jnp.zeros_like(picked))


def expand(expert_rows, gate_part, up_part):
    gate_proj = jnp.einsum(
        "rcd,df->rcf", expert_rows, gate_part, preferred_element_type=jnp.float32
    )
    up_proj = jnp.einsum("rcd,df->rcf", expert_rows, up_part, preferred_element_type=jnp.float32)
    return (jax.nn.silu(gate_proj) * up_proj).astype(jnp.bfloat16)


def meet(devices):
    barrier = pltpu.get_barrier_semaphore()
    for ep_to, tp_to in devices:
        pl.semaphore_signal(
            barrier, inc=1, device_id={"ep": ep_to, "tp": tp_to}, device_id_type=MESH
        )
    pl.semaphore_wait(barrier, len(devices))


def push(src, dst, send, recv, ep_to, tp_to):
    copy = pltpu.make_async_remote_copy(
        src_ref=src,
        dst_ref=dst,
        send_sem=send,
        recv_sem=recv,
        device_id={"ep": ep_to, "tp": tp_to},
        device_id_type=MESH,
    )
    copy.start()
    return copy


def fused_kernel(
    ep_count,
    q_ref, k_ref, v_ref, s_ref, rows_ref, ow_hbm, gw_hbm, uw_hbm, dw_hbm,
    mixed_ref, home_ref,
    ow, gw, uw, dw, qkv, shifts, gath, part, got_c, pair, got1, mid, got2, final,
    att, att_all, proj, got_o, pair_o, got_oy,
    send_a, recv_a, send_b, recv_b, send_r, recv_r, send_s, recv_s, own_sem, load_sem,
):
    e = lax.axis_index("ep")
    t = lax.axis_index("tp")
    g = e // 2
    x = e % 2
    y = t // 2
    c = t % 2
    e_x = g * 2 + (1 - x)
    t_y = (t + 2) % 4
    t_c = t + 1 - 2 * c
    t_yc = (t_c + 2) % 4
    block = q_ref.shape[0]
    width = q_ref.shape[1] // ep_count
    slots = rows_ref.shape[1]
    model = mixed_ref.shape[1]
    order = (0, 3, 1, 2)
    x_first = (0, 1)

    loads = []
    for n, (src, dst) in enumerate(((gw_hbm, gw), (uw_hbm, uw), (dw_hbm, dw), (ow_hbm, ow))):
        load = pltpu.make_async_copy(src, dst, load_sem.at[n])
        load.start()
        loads.append(load)
    owns = []

    def keep(src, dst):
        own = pltpu.make_async_copy(src, dst, own_sem.at[len(owns)])
        own.start()
        owns.append(own)
        return own

    mine = pl.ds(pl.multiple_of(e * width, width), width)
    here = pl.ds(pl.multiple_of(e * block, block), block)
    kept_rows = keep(rows_ref.at[g], gath.at[g, x, t])
    for i, ref in enumerate((q_ref, k_ref, v_ref)):
        keep(ref.at[:, mine], qkv.at[i, here])
    keep(s_ref.at[e], shifts.at[e])
    meet([((e + d) % ep_count, t) for d in range(1, ep_count)] + [(e, t_y), (e, t_c)])

    sends = []

    def send_rows(src, z, xi, ti, ep_to, tp_to):
        sends.append(
            push(
                src, gath.at[z, xi, ti], send_b.at[len(sends)], recv_b.at[z, xi, ti], ep_to, tp_to
            )
        )

    def forward(z, xi, ti, ep_to, tp_to):
        send_rows(gath.at[z, xi, ti], z, xi, ti, ep_to, tp_to)

    def arrived(z, xi, ti):
        place = gath.at[z, xi, ti]
        pltpu.make_async_copy(place, place, recv_b.at[z, xi, ti]).wait()

    for dz in (3, 1, 2):
        to = (g + dz) % GROUPS
        send_rows(rows_ref.at[to], g, x, t, to * 2 + x, t)
    for ep_to, tp_to in ((e_x, t), (e, t_y), (e, t_c)):
        send_rows(rows_ref.at[g], g, x, t, ep_to, tp_to)
    exchange = []

    def exchange_heads(distances):
        for d in distances:
            to = (e + d) % ep_count
            cols = pl.ds(pl.multiple_of(to * width, width), width)
            for i, ref in enumerate((q_ref, k_ref, v_ref)):
                exchange.append(
                    push(
                        ref.at[:, cols], qkv.at[i, here],
                        send_a.at[i, d - 1], recv_a.at[i, d - 1], to, t,
                    )
                )
            exchange.append(
                push(s_ref.at[to], shifts.at[e], send_a.at[3, d - 1], recv_a.at[3, d - 1], to, t)
            )

    exchange_heads(range(2, ep_count, 2))

    later_sends = []

    def go(src, dst, ep_to, tp_to):
        n = len(later_sends)
        copy = push(src, dst, send_s.at[n], recv_s.at[n], ep_to, tp_to)
        later_sends.append(copy)
        return copy

    def add(a, b):
        return (a.astype(jnp.float32) + b.astype(jnp.float32)).astype(jnp.bfloat16)

    def plane_of(dz):
        return (g + dz) % GROUPS

    def first_leg(dz):
        z = plane_of(dz)
        arrived(z, x, t)
        forward(z, x, t, e_x, t)
        forward(z, x, t, e, t_y)
        forward(z, x, t, e, t_c)

    def second_leg(dz):
        z = plane_of(dz)
        arrived(z, 1 - x, t)
        if dz in (0, 3):
            forward(z, 1 - x, t, e, t_y)
        forward(z, 1 - x, t, e, t_c)
        arrived(z, x, t_y)
        if dz not in (0, 3):
            forward(z, x, t_y, e_x, t)
        forward(z, x, t_y, e, t_c)

    def third_leg(dz):
        z = plane_of(dz)
        arrived(z, 1 - x, t_y)
        forward(z, 1 - x, t_y, e, t_c)

    lane = lax.broadcasted_iota(jnp.int32, (2 * 4 * slots, rows_ref.shape[2] - model), 1)
    chosen = (lane >= 3 * x) & (lane < 3 * x + 3)
    swaps = {}
    hops = {}
    ends = {}

    def experts(dz):
        z = plane_of(dz)
        for xi in (x, 1 - x):
            arrived(z, xi, t_c)
            arrived(z, xi, t_yc)
        rows = gath[z].reshape(2 * 4 * slots, rows_ref.shape[2])
        inputs = rows[:, :model]
        marks = rows[:, model:].astype(jnp.float32)
        scale = jnp.sum(jnp.where(chosen, marks, 0.0), axis=1, keepdims=True)
        gate = jnp.dot(inputs, gw[...], preferred_element_type=jnp.float32)
        up = jnp.dot(inputs, uw[...], preferred_element_type=jnp.float32)
        hidden = (gate / (1.0 + jnp.exp(-gate)) * up).astype(jnp.bfloat16)
        step = model // 4
        for n in range(4):
            cols = slice(n * step, (n + 1) * step)
            down = jnp.dot(hidden, dw[:, cols], preferred_element_type=jnp.float32)
            down = (down * scale).astype(jnp.bfloat16)
            for xi in range(2):
                for ti in range(4):
                    at = (xi * 4 + ti) * slots
                    part[dz, ti % 2, xi, ti // 2, :, cols] = down[at : at + slots]
        swaps[dz] = go(part.at[dz, 1 - c], got_c.at[dz], e, t_c)

    def pair_sum(dz):
        swaps[dz].wait_recv()
        pair[dz] = add(part[dz, c], got_c[dz])
        if dz in x_first:
            hops[dz] = go(pair.at[dz, 1 - x], got1.at[dz], e_x, t)
        else:
            hops[dz] = go(pair.at[dz, :, 1 - y], got1.at[dz], e, t_y)

    def middle_sum(dz):
        hops[dz].wait_recv()
        if dz in x_first:
            mid[dz] = add(pair[dz, x], got1[dz])
            ends[dz] = go(mid.at[dz, 1 - y], got2.at[dz], e, t_y)
        else:
            mid[dz] = add(pair[dz, :, y], got1[dz])
            ends[dz] = go(mid.at[dz, 1 - x], got2.at[dz], e_x, t)

    backs = []

    def send_home(dz):
        ends[dz].wait_recv()
        total = add(mid[dz, y if dz in x_first else x], got2[dz])
        if dz == 0:
            home_ref[g] = total
        else:
            final[dz] = total
            backs.append(go(final.at[dz], home_ref.at[g], plane_of(dz) * 2 + x, t))

    kept_rows.wait()
    second_leg(0)
    first_leg(3)
    first_leg(1)
    second_leg(3)
    third_leg(0)
    first_leg(2)
    second_leg(1)
    third_leg(3)
    for load in loads[:3]:
        load.wait()
    experts(0)
    second_leg(2)
    exchange_heads(range(1, ep_count, 2))
    third_leg(1)
    experts(3)
    third_leg(2)
    pair_sum(0)
    experts(1)
    pair_sum(3)
    experts(2)
    pair_sum(1)
    pair_sum(2)
    for copy in exchange:
        copy.wait()
    for own in owns[1:]:
        own.wait()
    blocks = att.shape[0] // TILE
    half = blocks // 2
    for i in range(blocks - 1, half - 1, -1):
        stick_block(i, qkv, shifts, att)
    middle_sum(0)
    middle_sum(3)
    for i in range(half - 1, -1, -1):
        stick_block(i, qkv, shifts, att)
    regroups = []
    for d in range(1, ep_count):
        to = (e + d) % ep_count
        rows = pl.ds(pl.multiple_of(to * block, block), block)
        regroups.append(
            push(
                att.at[rows], att_all.at[:, mine], send_r.at[d - 1], recv_r.at[d - 1], to, t
            )
        )
    own_heads = keep(att.at[here], att_all.at[:, mine])
    middle_sum(1)
    middle_sum(2)
    for dz in (3, 1, 2, 0):
        send_home(dz)
    for copy in regroups:
        copy.wait()
    own_heads.wait()
    loads[3].wait()
    sub = mixed_ref.shape[0]
    chunk = 512

    def project(n, carry):
        cols = pl.ds(pl.multiple_of(n * chunk, chunk), chunk)
        value = jnp.dot(att_all[...], ow[:, cols], preferred_element_type=jnp.float32)
        value = value.astype(jnp.bfloat16)
        for ti in range(4):
            proj[ti % 2, ti // 2, :, cols] = value[ti * sub : (ti + 1) * sub]
        return carry

    lax.fori_loop(0, model // chunk, project, 0)
    swap_o = go(proj.at[1 - c], got_o, e, t_c)
    swap_o.wait_recv()
    pair_o[1 - y] = add(proj[c, 1 - y], got_o[1 - y])
    hop_o = go(pair_o.at[1 - y], got_oy, e, t_y)
    pair_o[y] = add(proj[c, y], got_o[y])
    hop_o.wait_recv()
    mixed_ref[...] = add(pair_o[y], got_oy[...])
    for copy in backs:
        copy.wait_recv()
    for copy in sends + later_sends:
        copy.wait_send()


def stick_block(i, qkv, shifts, out_ref):
    width = qkv.shape[2]
    heads = width // HEAD
    per = shifts.shape[2]
    score_scale = HEAD ** (-0.5)
    lane = lax.broadcasted_iota(jnp.int32, (TILE, width), 1) // HEAD
    strict = lax.broadcasted_iota(jnp.int32, (TILE, TILE), 1) < lax.broadcasted_iota(
        jnp.int32, (TILE, TILE), 0
    )
    tri = jnp.where(
        lax.broadcasted_iota(jnp.int32, (TILE, TILE), 0)
        > lax.broadcasted_iota(jnp.int32, (TILE, TILE), 1),
        1.0,
        0.0,
    ).astype(jnp.bfloat16)
    q_all = qkv[0, i * TILE : (i + 1) * TILE]
    q_heads = [jnp.where(lane == h, q_all, jnp.zeros_like(q_all)) for h in range(heads)]
    running = [jnp.zeros((TILE, width), jnp.float32) for _ in range(heads)]
    logsum = [jnp.zeros((TILE, 1), jnp.float32) for _ in range(heads)]
    for j in range(i, -1, -1):
        k_all = qkv[1, j * TILE : (j + 1) * TILE]
        v_all = qkv[2, j * TILE : (j + 1) * TILE]
        for h in range(heads):
            shift = jnp.concatenate(
                [shifts[j * (TILE // per) + p, h : h + 1] for p in range(TILE // per)], axis=1
            )
            score = (
                lax.dot_general(
                    q_heads[h],
                    k_all,
                    (((1,), (1,)), ((), ())),
                    preferred_element_type=jnp.float32,
                )
                * score_scale
                + shift
            )
            tail = jnp.log(1.0 + jnp.exp(-jnp.abs(score)))
            log_take = jnp.minimum(score, 0.0) - tail
            log_keep = -jnp.maximum(score, 0.0) - tail
            if i == j:
                log_keep = jnp.where(strict, log_keep, 0.0)
            high = log_keep.astype(jnp.bfloat16)
            low = (log_keep - high.astype(jnp.float32)).astype(jnp.bfloat16)
            later = jnp.dot(high, tri, preferred_element_type=jnp.float32) + jnp.dot(
                low, tri, preferred_element_type=jnp.float32
            )
            weight = jnp.exp(log_take + later + logsum[h])
            if i == j:
                weight = jnp.where(strict, weight, 0.0)
            running[h] = running[h] + jnp.dot(
                weight.astype(jnp.bfloat16), v_all, preferred_element_type=jnp.float32
            )
            logsum[h] = logsum[h] + later[:, :1] + log_keep[:, :1]
    result = running[0]
    for h in range(1, heads):
        result = jnp.where(lane == h, running[h], result)
    out_ref[i * TILE : (i + 1) * TILE] = result.astype(jnp.bfloat16)


def fused(q, k, v, shift_rows, rows, out_w, gate_w, up_w, down_w, ep_count, tp_count):
    block = q.shape[0]
    width = q.shape[1] // ep_count
    slots, row_width = rows.shape[1:]
    model = out_w.shape[1]
    sub = block // tp_count
    vmem_spec = pl.BlockSpec(memory_space=pltpu.VMEM)
    any_spec = pl.BlockSpec(memory_space=pl.ANY)
    bf = jnp.bfloat16
    dma = pltpu.SemaphoreType.DMA
    one = (slots, model)

    def kernel(*refs):
        fused_kernel(ep_count, *refs)

    return pl.pallas_call(
        kernel,
        out_shape=(
            jax.ShapeDtypeStruct((sub, model), bf),
            jax.ShapeDtypeStruct((GROUPS, *one), bf),
        ),
        in_specs=[vmem_spec] * 5 + [any_spec] * 4,
        out_specs=(vmem_spec,) * 2,
        scratch_shapes=[
            pltpu.VMEM(out_w.shape, bf),
            pltpu.VMEM(gate_w.shape, bf),
            pltpu.VMEM(up_w.shape, bf),
            pltpu.VMEM(down_w.shape, bf),
            pltpu.VMEM((3, block * ep_count, width), bf),
            pltpu.VMEM(shift_rows.shape, jnp.float32),
            pltpu.VMEM((GROUPS, 2, tp_count, slots, row_width), bf),
            pltpu.VMEM((GROUPS, 2, 2, 2, *one), bf),
            pltpu.VMEM((GROUPS, 2, 2, *one), bf),
            pltpu.VMEM((GROUPS, 2, 2, *one), bf),
            pltpu.VMEM((GROUPS, 2, *one), bf),
            pltpu.VMEM((GROUPS, 2, *one), bf),
            pltpu.VMEM((GROUPS, *one), bf),
            pltpu.VMEM((GROUPS, *one), bf),
            pltpu.VMEM((block * ep_count, width), bf),
            pltpu.VMEM(q.shape, bf),
            pltpu.VMEM((2, 2, sub, model), bf),
            pltpu.VMEM((2, sub, model), bf),
            pltpu.VMEM((2, sub, model), bf),
            pltpu.VMEM((sub, model), bf),
            dma((4, ep_count - 1)),
            dma((4, ep_count - 1)),
            dma((31,)),
            dma((GROUPS, 2, tp_count)),
            dma((ep_count - 1,)),
            dma((ep_count - 1,)),
            dma((17,)),
            dma((17,)),
            dma((6,)),
            dma((4,)),
        ],
        compiler_params=pltpu.CompilerParams(
            collective_id=0, has_side_effects=True, vmem_limit_bytes=60000 * 1024
        ),
    )(q, k, v, shift_rows, rows, out_w, gate_w, up_w, down_w)


def shards_paired(
    queries, key_rows, value_rows, key_shift, out_weight, routed_rows, expert_ids,
    route_weights, gate_weight, up_weight, down_weight,
):
    ep_count = lax.axis_size("ep")
    tp_count = lax.axis_size("tp")
    local_rows = queries.shape[0]
    sub = local_rows // tp_count
    slots = 4 * sub // ep_count
    model_width = routed_rows.shape[1]
    column = lax.axis_index("tp")

    ids = lax.dynamic_slice_in_dim(expert_ids, column * sub, sub, 0)
    own_rows = lax.dynamic_slice_in_dim(routed_rows, column * sub, sub, 0)
    group = ids[:, 0] // 2
    token = jnp.arange(sub, dtype=jnp.int32)
    earlier = (group[:, None] == group[None, :]) & (token[None, :] < token[:, None])
    place = group * slots + jnp.sum(earlier.astype(jnp.int32), axis=1)
    pick = place[None, :] == jnp.arange(GROUPS * slots, dtype=jnp.int32)[:, None]
    packed = jnp.dot(pick.astype(jnp.bfloat16), own_rows, preferred_element_type=jnp.float32)
    side = [
        jnp.sum(jnp.where(ids % 2 == s, route_weights, 0.0), axis=1) for s in range(2)
    ]
    pieces = []
    for weights in side:
        spread_w = jnp.sum(jnp.where(pick, weights[None, :], 0.0), axis=1)
        first = lax.reduce_precision(spread_w, 8, 7)
        second = lax.reduce_precision(spread_w - first, 8, 7)
        pieces += [first, second, spread_w - first - second]
    extra = jnp.pad(jnp.stack(pieces, axis=1), ((0, 0), (0, 128 - len(pieces))))
    rows = jnp.concatenate([packed.astype(jnp.bfloat16), extra.astype(jnp.bfloat16)], axis=1)
    rows = rows.reshape(GROUPS, slots, model_width + 128)

    per = key_shift.shape[1] // ep_count
    shift_rows = key_shift.astype(jnp.float32).T.reshape(ep_count, per, local_rows)
    shift_rows = jnp.pad(shift_rows, ((0, 0), (0, -per % 8), (0, 0)))
    mixed_rows, home = fused(
        queries, key_rows, value_rows, shift_rows, rows,
        out_weight, gate_weight[0], up_weight[0], down_weight[0], ep_count, tp_count,
    )
    home = home.reshape(GROUPS * slots, model_width)
    routed_out = jnp.dot(
        pick.T.astype(jnp.bfloat16), home, preferred_element_type=jnp.float32
    ).astype(jnp.bfloat16)
    return (mixed_rows, routed_out)


def shards(
    queries,
    key_rows,
    value_rows,
    key_shift,
    out_weight,
    routed_rows,
    expert_ids,
    route_weights,
    gate_weight,
    up_weight,
    down_weight,
):
    tp_count = lax.axis_size("tp")
    local_rows = queries.shape[0]
    heads_here = key_shift.shape[1]
    key_all, value_all, shift_all = (
        lax.all_gather(key_rows, "ep", axis=0, tiled=True),
        lax.all_gather(value_rows, "ep", axis=0, tiled=True),
        lax.all_gather(key_shift, "ep", axis=0, tiled=True),
    )
    first_pos = lax.axis_index("ep") * local_rows
    attended = stick_attend(
        queries.reshape(local_rows, heads_here, HEAD), key_all, value_all, shift_all, first_pos
    )
    mixed_rows = lax.psum_scatter(
        jnp.dot(attended, out_weight, preferred_element_type=jnp.float32).astype(jnp.bfloat16),
        "tp",
        scatter_dimension=0,
        tiled=True,
    )
    expert_count = lax.axis_size("ep")
    sub_rows = local_rows // tp_count
    capacity = 4 * sub_rows // expert_count
    model_width = routed_rows.shape[1]
    column = lax.axis_index("tp")
    own_ids = lax.dynamic_slice_in_dim(expert_ids, column * sub_rows, sub_rows, 0).reshape(
        1, sub_rows * 2
    )
    own_slot = slot_numbers(own_ids, expert_count)[0]
    own_dest = own_ids[0] * capacity + own_slot
    own_input = lax.dynamic_slice_in_dim(routed_rows, column * sub_rows, sub_rows, 0)
    outgoing = pack_rows(own_input, own_dest, expert_count * capacity).reshape(
        expert_count, capacity, model_width
    )
    arrived = lax.all_to_all(outgoing, "ep", split_axis=0, concat_axis=0, tiled=True)
    hidden = expand(lax.all_gather(arrived, "tp", axis=1, tiled=True), gate_weight[0], up_weight[0])
    unit_count = hidden.shape[2]
    ordered = jnp.transpose(
        hidden.reshape(expert_count, tp_count, capacity, unit_count), (1, 0, 2, 3)
    )
    ordered = ordered.reshape(tp_count * expert_count * capacity, unit_count)
    partial_value = lax.psum_scatter(
        jnp.dot(ordered, down_weight[0], preferred_element_type=jnp.float32).astype(jnp.bfloat16),
        "tp",
        scatter_dimension=0,
        tiled=True,
    )
    returned = lax.all_to_all(
        partial_value.reshape(expert_count, capacity, model_width),
        "ep",
        split_axis=0,
        concat_axis=0,
        tiled=True,
    )
    picked = jnp.take(returned.reshape(expert_count * capacity, model_width), own_dest, axis=0)
    picked = picked.reshape(sub_rows, 2, model_width).astype(jnp.float32)
    routed_out = (
        picked[:, 0] * route_weights[:, 0:1] + picked[:, 1] * route_weights[:, 1:2]
    ).astype(jnp.bfloat16)
    return (mixed_rows, routed_out)


def solution(mesh):
    paired = mesh.shape["ep"] == 2 * GROUPS and mesh.shape["tp"] == 4
    return jax.shard_map(
        shards_paired if paired else shards,
        mesh=mesh,
        in_specs=(
            P("ep", "tp"),
            P("ep", "tp"),
            P("ep", "tp"),
            P("ep", "tp"),
            P("tp", None),
            P("ep", None),
            P("ep", None),
            P(("ep", "tp"), None),
            P("ep", None, "tp"),
            P("ep", None, "tp"),
            P("ep", "tp", None),
        ),
        out_specs=(P(("ep", "tp"), None), P(("ep", "tp"), None)),
        check_vma=False,
    )
```
